512 devices in a mesh: ep: 32 (over z, core), tp: 16 (over y, x).
Axes of the slice: x: 4, y: 4, z: 16, core: 2. Of those that a mesh axis runs over, the one named last changes fastest.
Arguments:
- tokens: bfloat16 [1024, 4096], P('ep'), may hold values from -6 to 6
- recur_state: float32 [1024, 4096], P('ep', 'tp'), may hold values from -6 to 6
- conv_state: bfloat16 [1024, 3, 4096], P('ep', None, 'tp'), may hold values from -6 to 6
- mix_gain: float32 [4096], replicated, may hold values from 0.1 to 1.9
- in_weight: bfloat16 [4096, 4096], P('ep', 'tp'), may hold values from -0.09375 to 0.09375
- gate_weight: bfloat16 [4096, 4096], P('ep', 'tp'), may hold values from -0.09375 to 0.09375
- conv_taps: float32 [4, 4096], P(None, 'tp'), may hold values from -3 to 3
- recur_gate_blocks: bfloat16 [64, 64, 64], P('tp'), may hold values from -0.75 to 0.75
- input_gate_blocks: bfloat16 [64, 64, 64], P('tp'), may hold values from -0.75 to 0.75
- decay_rate: float32 [4096], P('tp'), may hold values from 0.01 to 0.4
- out_weight: bfloat16 [4096, 4096], P('tp', 'ep'), may hold values from -0.09375 to 0.09375
- ffn_gain: float32 [4096], replicated, may hold values from 0.1 to 1.9
- router_weight: bfloat16 [4096, 32], replicated, may hold values from -0.09375 to 0.09375
- routes: int32 [1024, 2], P('ep'), may hold values from 0 to 31, as said below
- expert_gate: bfloat16 [32, 4096, 2048], P('ep', None, 'tp'), may hold values from -0.09375 to 0.09375
- expert_up: bfloat16 [32, 4096, 2048], P('ep', None, 'tp'), may hold values from -0.09375 to 0.09375
- expert_down: bfloat16 [32, 2048, 4096], P('ep', 'tp'), may hold values from -0.125 to 0.125
- dense_gate: bfloat16 [4096, 2048], P('ep', 'tp'), may hold values from -0.09375 to 0.09375
- dense_up: bfloat16 [4096, 2048], P('ep', 'tp'), may hold values from -0.09375 to 0.09375
- dense_down: bfloat16 [2048, 4096], P('tp', 'ep'), may hold values from -0.125 to 0.125
- branch_gate: bfloat16 [4096], replicated, may hold values from -0.09375 to 0.09375
Outputs:
- layer_out: bfloat16 [1024, 4096], P('ep')
- new_state: float32 [1024, 4096], P('ep', 'tp')
- new_conv_state: bfloat16 [1024, 3, 4096], P('ep', None, 'tp')
The draws below stay inside these ranges and needn't reach their ends.
Inputs may be any that keep to these rules, and one draw needn't show every extreme that they name: `routes`: A row names two different experts of one group: both have the same e // 4. In the rows of one index of ep no expert is named more than 4 times, and in every draw some expert is named exactly 4 times by the rows of every index of ep.
All inputs are finite; a program needn't handle non-finite values.
Results may differ from the reference program's by a relative error of at most 0.023.
Values may be sent and summed in bfloat16 or wider, within the bound.
No kernel may reach another device: no remote copies, remote signals or barrier semaphores. Data moves between devices by JAX's collectives and lax.ppermute only.
A program may use at most 64 MiB of HBM per device.

```python
import math
import jax
import jax.numpy as jnp
from jax import lax

D = 4096
D_A = 4096
BLOCK = 64
FF = 2048
FFD = 2048
CONV_W = 4
TOP_K = 2
E_PER_GROUP = 4
B_DEV = 32
B = 1024
EXPERTS = 32
CAP = 4
H_A = 64
N_EP = 32
N_TP = 16


def draw_routes(key, part):
    group_count = EXPERTS // E_PER_GROUP
    group_tokens = 2 * CAP
    slot_count = group_count * group_tokens
    base_group = jax.random.randint(jax.random.fold_in(key, 11), (), 0, group_count)

    def one_block(block):
        block_key = jax.random.fold_in(key, 1000 + block)
        full_group = (block + base_group) % group_count
        scores = jax.random.randint(jax.random.fold_in(block_key, 1), (slot_count,), 0, 1 << 20)
        slot_index = jnp.arange(slot_count, dtype=jnp.int32)
        keyed = jnp.where(slot_index // group_tokens == full_group, 0, scores + 1) * slot_count + slot_index
        chosen = jnp.argsort(keyed)[:B_DEV]
        chosen = chosen[jax.random.permutation(jax.random.fold_in(block_key, 2), B_DEV)]
        group = chosen // group_tokens
        pair = chosen % group_tokens
        member_scores = jax.random.randint(jax.random.fold_in(block_key, 3), (group_count, E_PER_GROUP), 0, 1 << 20) * E_PER_GROUP + jnp.arange(E_PER_GROUP, dtype=jnp.int32)[None, :]
        members = jnp.argsort(member_scores, axis=1).astype(jnp.int32)
        first = members[group, 2 * pair % E_PER_GROUP]
        second = members[group, (2 * pair + 1) % E_PER_GROUP]
        return jnp.stack([group * E_PER_GROUP + first, group * E_PER_GROUP + second], axis=1).astype(jnp.int32)
    return jax.vmap(one_block)(jnp.arange(N_EP, dtype=jnp.int32)).reshape(N_EP * B_DEV, 2)


def block_levels(stream_key, dims, cuts, low, high):
    loudness = 1.0
    for axis_at, blocks in cuts:
        draws = jax.random.uniform(jax.random.fold_in(jax.random.fold_in(stream_key, 6), axis_at), (blocks,), jnp.float32, low / len(cuts), high / len(cuts))
        loudness = loudness * jnp.repeat(jnp.exp(draws), dims[axis_at] // blocks).reshape((-1,) + (1,) * (len(dims) - 1 - axis_at))
    return loudness


def normal_values(stream_key, shape, width, reach, split=(), held_as=jnp.bfloat16):
    entries = width * jax.random.normal(stream_key, shape, jnp.float32)
    if split:
        entries = entries * block_levels(stream_key, shape, split, -0.22, 0.18)
    return jnp.clip(entries, -reach, reach).astype(held_as)


def setup_inputs(seed: int = 0) -> dict:
    streams_of = jax.random.split(jax.random.key(seed), 22)
    tokens = normal_values(streams_of[0], (B, D), 1.0, 6.0, ((0, 32),))
    recur_state = normal_values(streams_of[1], (B, D_A), 1.0, 6.0, ((0, 32), (1, 16)), jnp.float32)
    conv_state = normal_values(streams_of[2], (B, CONV_W - 1, D_A), 1.0, 6.0, ((0, 32), (2, 16)))
    mix_gain = jnp.clip(1.0 + 0.18 * jax.random.normal(streams_of[3], (D,), jnp.float32), 0.1, 1.9)
    in_weight = normal_values(streams_of[4], (D, D_A), D ** -0.5, 0.09375, ((0, 32), (1, 16)))
    gate_weight = normal_values(streams_of[5], (D, D_A), D ** -0.5, 0.09375, ((0, 32), (1, 16)))
    conv_taps = normal_values(streams_of[6], (CONV_W, D_A), 0.5, 3.0, ((1, 16),), jnp.float32)
    recur_gate_blocks = normal_values(streams_of[7], (H_A, BLOCK, BLOCK), BLOCK ** -0.5, 0.75, ((0, 16),))
    input_gate_blocks = normal_values(streams_of[8], (H_A, BLOCK, BLOCK), BLOCK ** -0.5, 0.75, ((0, 16),))
    decay_rate = jnp.clip(jnp.exp(math.log(0.4) - 3.6888795 * jax.random.uniform(streams_of[9], (D_A,), jnp.float32) ** block_levels(streams_of[9], (D_A,), ((0, 16),), -0.2, 0.2)), 0.01, 0.4)
    out_weight = normal_values(streams_of[10], (D_A, D), D_A ** -0.5, 0.09375, ((0, 16), (1, 32)))
    ffn_gain = jnp.clip(1.0 + 0.18 * jax.random.normal(streams_of[11], (D,), jnp.float32), 0.1, 1.9)
    router_weight = normal_values(streams_of[12], (D, EXPERTS), D ** -0.5, 0.09375)
    routes = draw_routes(jax.random.fold_in(streams_of[21], 71), 0)
    expert_gate = normal_values(streams_of[14], (EXPERTS, D, FF), D ** -0.5, 0.09375, ((0, 32), (2, 16)))
    expert_up = normal_values(streams_of[15], (EXPERTS, D, FF), D ** -0.5, 0.09375, ((0, 32), (2, 16)))
    expert_down = normal_values(streams_of[16], (EXPERTS, FF, D), FF ** -0.5, 0.125, ((0, 32), (1, 16)))
    dense_gate = normal_values(streams_of[17], (D, FFD), D ** -0.5, 0.09375, ((0, 32), (1, 16)))
    dense_up = normal_values(streams_of[18], (D, FFD), D ** -0.5, 0.09375, ((0, 32), (1, 16)))
    dense_down = normal_values(streams_of[19], (FFD, D), FFD ** -0.5, 0.125, ((0, 16), (1, 32)))
    branch_gate = normal_values(streams_of[20], (D,), D ** -0.5, 0.09375)
    return dict(tokens=tokens, recur_state=recur_state, conv_state=conv_state, mix_gain=mix_gain, in_weight=in_weight, gate_weight=gate_weight, conv_taps=conv_taps, recur_gate_blocks=recur_gate_blocks, input_gate_blocks=input_gate_blocks, decay_rate=decay_rate, out_weight=out_weight, ffn_gain=ffn_gain, router_weight=router_weight, routes=routes, expert_gate=expert_gate, expert_up=expert_up, expert_down=expert_down, dense_gate=dense_gate, dense_up=dense_up, dense_down=dense_down, branch_gate=branch_gate)


epsilon = 1e-06
decay_scale = 8.0

def rms_scale(rows, gain):
    values = rows.astype(jnp.float32)
    inverse = lax.rsqrt(lax.optimization_barrier(jnp.mean(values * values, axis=-1, keepdims=True)) + epsilon)
    return (values * inverse * gain.astype(jnp.float32)).astype(jnp.bfloat16)

def grouped_product(left, right, groups):
    rows = left.shape[0]
    inner = left.shape[1] // groups
    parts = jnp.einsum('rtf,tfd->trd', left.astype(jnp.float32).reshape(rows, groups, inner), right.astype(jnp.float32).reshape(groups, inner, right.shape[1]))
    rounded = lax.optimization_barrier(parts.astype(jnp.bfloat16))
    return lax.optimization_barrier(jnp.sum(rounded.astype(jnp.float32), axis=0))

def slot_table(routes):
    pairs = routes.reshape(N_EP, B_DEV * TOP_K)
    expert_ids = jnp.arange(EXPERTS, dtype=jnp.int32)
    onehot = (pairs[:, :, None] == expert_ids[None, None, :]).astype(jnp.int32)
    before = jnp.cumsum(onehot, axis=1) - onehot
    rank = lax.optimization_barrier(jnp.sum(before * onehot, axis=2))
    return (pairs * CAP + rank).reshape(N_EP * B_DEV, TOP_K).astype(jnp.int32)

def reference(tokens, recur_state, conv_state, mix_gain, in_weight, gate_weight, conv_taps, recur_gate_blocks, input_gate_blocks, decay_rate, out_weight, ffn_gain, router_weight, routes, expert_gate, expert_up, expert_down, dense_gate, dense_up, dense_down, branch_gate):
    batch_rows = tokens.shape[0]
    normed = rms_scale(tokens, mix_gain)
    x_branch = jnp.dot(normed, in_weight, preferred_element_type=jnp.float32).astype(jnp.bfloat16)
    gate_branch = jnp.dot(normed, gate_weight, preferred_element_type=jnp.float32).astype(jnp.bfloat16)
    window = jnp.concatenate([conv_state, x_branch[:, None, :]], axis=1)
    conv_out = lax.optimization_barrier(jnp.sum(window.astype(jnp.float32) * conv_taps.astype(jnp.float32)[None], axis=1)).astype(jnp.bfloat16)
    new_conv_state = window[:, 1:, :]
    blocks = conv_out.astype(jnp.float32).reshape(batch_rows, H_A, BLOCK)
    recur_gate = jax.nn.sigmoid(jnp.einsum('bhi,hij->bhj', blocks, recur_gate_blocks.astype(jnp.float32)).reshape(batch_rows, D_A))
    input_gate = jax.nn.sigmoid(jnp.einsum('bhi,hij->bhj', blocks, input_gate_blocks.astype(jnp.float32)).reshape(batch_rows, D_A))
    log_decay = -decay_scale * recur_gate * decay_rate
    new_state = jnp.exp(log_decay) * recur_state + jnp.sqrt(-jnp.expm1(2.0 * log_decay)) * input_gate * conv_out.astype(jnp.float32)
    mixer_rows = (new_state * jax.nn.gelu(gate_branch.astype(jnp.float32))).astype(jnp.bfloat16)
    mixed = grouped_product(mixer_rows, out_weight, N_TP)
    resid = (tokens.astype(jnp.float32) + mixed).astype(jnp.bfloat16)
    normed_ffn = rms_scale(resid, ffn_gain)
    router_logits = jnp.dot(normed_ffn, router_weight, preferred_element_type=jnp.float32)
    picked = jnp.take_along_axis(router_logits, routes, axis=1)
    route_weight = jax.nn.sigmoid(picked - picked[:, ::-1]).astype(jnp.bfloat16)
    slots = slot_table(routes)
    global_token = jnp.arange(batch_rows, dtype=jnp.int32)
    source = global_token // B_DEV
    owner = jnp.full((N_EP, EXPERTS * CAP), -1, jnp.int32)
    owner = owner.at[jnp.repeat(source[:, None], TOP_K, axis=1), slots].set(jnp.repeat(global_token[:, None], TOP_K, axis=1))
    table = owner.reshape(N_EP, EXPERTS, CAP).transpose(1, 0, 2).reshape(EXPERTS, N_EP * CAP)

    def serve(item):
        token_index, gate_matrix, up_matrix, down_matrix = item
        valid = token_index >= 0
        rows = jnp.where(valid[:, None], normed_ffn[jnp.maximum(token_index, 0)], jnp.zeros((), jnp.bfloat16))
        first = jnp.dot(rows, gate_matrix, preferred_element_type=jnp.float32)
        second = jnp.dot(rows, up_matrix, preferred_element_type=jnp.float32)
        act = (jax.nn.silu(first) * second).astype(jnp.bfloat16)
        return grouped_product(act, down_matrix, N_TP).astype(jnp.bfloat16)
    expert_rows = lax.map(serve, (table, expert_gate, expert_up, expert_down))
    flat_rows = expert_rows.reshape(EXPERTS * N_EP * CAP, D)
    flat_index = slots // CAP * (N_EP * CAP) + source[:, None] * CAP + slots % CAP
    chosen = flat_rows[flat_index].astype(jnp.float32)
    moe = lax.optimization_barrier(jnp.sum(route_weight.astype(jnp.float32)[:, :, None] * chosen, axis=1))
    dense_first = jnp.dot(normed_ffn, dense_gate, preferred_element_type=jnp.float32)
    dense_second = jnp.dot(normed_ffn, dense_up, preferred_element_type=jnp.float32)
    dense_act = (jax.nn.silu(dense_first) * dense_second).astype(jnp.bfloat16)
    dense_sum = grouped_product(dense_act, dense_down, N_TP)
    branch_weight = jax.nn.sigmoid(jnp.dot(normed_ffn, branch_gate, preferred_element_type=jnp.float32))
    layer_out = (resid.astype(jnp.float32) + moe + branch_weight[:, None] * dense_sum).astype(jnp.bfloat16)
    return (layer_out, new_state, new_conv_state)
```

```python
import jax
import jax.numpy as jnp
from jax import lax
from jax.sharding import Mesh
from jax.sharding import PartitionSpec as P

TOP_K = 2
EP = ("ep_0", "ep_1")


epsilon = 1e-06
decay_scale = 8.0


def exchange(pieces, axis):
    return lax.all_to_all(pieces, axis, split_axis=0, concat_axis=0, tiled=True)


def copies_to_all(value, axis):
    return exchange(jnp.broadcast_to(value, (lax.axis_size(axis), *value.shape)), axis)


def features_cut(rows, devices):
    count, width = rows.shape
    return rows.reshape(count, devices, width // devices).swapaxes(0, 1)


def features_joined(pieces):
    devices, count, share = pieces.shape
    return pieces.swapaxes(0, 1).reshape(count, devices * share)


def rms_scale(rows, gain):
    values = rows.astype(jnp.float32)
    inverse = lax.rsqrt(jnp.mean(values * values, axis=-1, keepdims=True) + epsilon)
    return (values * inverse * gain).astype(jnp.bfloat16)


def dot(left, right):
    return jnp.dot(left, right, preferred_element_type=jnp.float32)


def lane_blocks(weight, lanes):
    return [weight[:, at : at + lanes] for at in range(0, weight.shape[1], lanes)]


def on_device(
    tokens,
    recur_state,
    conv_state,
    mix_gain,
    in_weight,
    gate_weight,
    conv_taps,
    recur_gate_blocks,
    input_gate_blocks,
    decay_rate,
    out_weight,
    ffn_gain,
    router_weight,
    routes,
    expert_gate,
    expert_up,
    expert_down,
    dense_gate,
    dense_up,
    dense_down,
    branch_gate,
):
    batch_rows, width = tokens.shape
    depth, channels = in_weight.shape
    lanes = out_weight.shape[1]
    columns = lax.axis_size("tp")
    share = width // columns
    parts = [*lane_blocks(in_weight, lanes), *lane_blocks(gate_weight, lanes), out_weight, dense_gate, dense_up, dense_down]
    whole = lax.all_gather(jnp.concatenate(parts, axis=0), EP)
    pieces, at = [], 0
    for part in parts:
        pieces.append(whole[:, at : at + part.shape[0]])
        at += part.shape[0]
    per = channels // lanes
    by_rows = lambda piece: piece.reshape(-1, lanes)
    by_columns = lambda piece: piece.swapaxes(0, 1).reshape(piece.shape[1], -1)
    in_whole = jnp.concatenate([by_rows(p) for p in pieces[:per]], axis=1)
    gate_whole = jnp.concatenate([by_rows(p) for p in pieces[per : 2 * per]], axis=1)
    out_piece, dense_gate_piece, dense_up_piece, dense_down_piece = pieces[2 * per :]

    normed = rms_scale(tokens, mix_gain)
    x_branch = dot(normed, in_whole).astype(jnp.bfloat16)
    gate_branch = dot(normed, gate_whole).astype(jnp.bfloat16)
    window = jnp.concatenate([conv_state, x_branch[:, None, :]], axis=1)
    conv_out = jnp.sum(window.astype(jnp.float32) * conv_taps[None], axis=1).astype(jnp.bfloat16)
    new_conv_state = window[:, 1:, :]
    blocks = conv_out.reshape(batch_rows, recur_gate_blocks.shape[0], recur_gate_blocks.shape[1])

    def block_gate(maps):
        sums = jnp.einsum("bhi,hij->bhj", blocks, maps, preferred_element_type=jnp.float32)
        return jax.nn.sigmoid(sums.reshape(batch_rows, channels))

    recur_gate = block_gate(recur_gate_blocks)
    input_gate = block_gate(input_gate_blocks)
    log_decay = -decay_scale * recur_gate * decay_rate
    new_state = jnp.exp(log_decay) * recur_state + jnp.sqrt(
        -jnp.expm1(2.0 * log_decay)
    ) * input_gate * conv_out.astype(jnp.float32)
    mixer_rows = (new_state * jax.nn.gelu(gate_branch.astype(jnp.float32))).astype(jnp.bfloat16)
    mixer_part = dot(mixer_rows, by_columns(out_piece)).astype(jnp.bfloat16)

    mixed_share = exchange(features_cut(mixer_part, columns), "tp").astype(jnp.float32).sum(axis=0)
    own_tokens = lax.dynamic_slice_in_dim(tokens, lax.axis_index("tp") * share, share, 1)
    resid_share = (own_tokens.astype(jnp.float32) + mixed_share).astype(jnp.bfloat16)

    experts = router_weight.shape[1]
    capacity = 2 * batch_rows * TOP_K // experts
    flat_ids = routes.reshape(batch_rows * TOP_K)
    onehot = (
        flat_ids[:, None] == lax.broadcasted_iota(jnp.int32, (batch_rows * TOP_K, experts), 1)
    ).astype(jnp.int32)
    rank = jnp.sum((jnp.cumsum(onehot, axis=0) - onehot) * onehot, axis=1)
    slot_of = (flat_ids * capacity + rank).reshape(batch_rows, TOP_K)
    slot_rows = lax.broadcasted_iota(jnp.int32, (experts * capacity, batch_rows), 0)
    slot_cols = lax.broadcasted_iota(jnp.int32, (batch_rows, experts * capacity), 1)
    dispatch = jnp.zeros((experts * capacity, batch_rows), jnp.bfloat16)
    for pick in range(TOP_K):
        dispatch = dispatch + (slot_rows == slot_of[None, :, pick]).astype(jnp.bfloat16)

    outgoing = dot(dispatch, resid_share).astype(jnp.bfloat16).reshape(experts, capacity, share)
    arrived = exchange(outgoing, EP)
    sources, items, _ = arrived.shape
    slots = sources * items
    both = jnp.concatenate([arrived.reshape(slots, share), resid_share], axis=0)
    all_rows = features_joined(copies_to_all(both, "tp"))
    all_normed = rms_scale(all_rows, ffn_gain)
    rows, normed_ffn = all_normed[:slots], all_normed[slots:]

    act = (jax.nn.silu(dot(rows, expert_gate[0])) * dot(rows, expert_up[0])).astype(jnp.bfloat16)
    expert_part = dot(act, expert_down[0]).astype(jnp.bfloat16)
    dense_first = dot(normed_ffn, by_rows(dense_gate_piece))
    dense_second = dot(normed_ffn, by_rows(dense_up_piece))
    dense_act = (jax.nn.silu(dense_first) * dense_second).astype(jnp.bfloat16)
    dense_part = dot(dense_act, by_columns(dense_down_piece)).astype(jnp.bfloat16)
    parts_cut = features_cut(jnp.concatenate([expert_part, dense_part], axis=0), columns)
    sums = exchange(parts_cut, "tp").astype(jnp.float32).sum(axis=0)
    total, dense_share = sums[:slots].astype(jnp.bfloat16), sums[slots:]

    router_logits = dot(normed_ffn, router_weight)
    expert_ids = lax.broadcasted_iota(jnp.int32, (batch_rows, TOP_K, experts), 2)
    picked = jnp.sum(
        jnp.where(routes[:, :, None] == expert_ids, router_logits[:, None, :], 0.0), axis=2
    )
    route_weight = jax.nn.sigmoid(picked - picked[:, ::-1]).astype(jnp.bfloat16)
    combine = jnp.zeros((batch_rows, experts * capacity), jnp.bfloat16)
    for pick in range(TOP_K):
        combine = combine + jnp.where(
            slot_cols == slot_of[:, pick : pick + 1],
            route_weight[:, pick : pick + 1],
            jnp.zeros((), jnp.bfloat16),
        )
    branch_weight = jax.nn.sigmoid(dot(normed_ffn, branch_gate))

    returned = exchange(total.reshape(sources, items, share), EP)
    moe = dot(combine, returned.reshape(experts * capacity, share))
    out_share = (
        resid_share.astype(jnp.float32) + moe + branch_weight[:, None] * dense_share
    ).astype(jnp.bfloat16)
    layer_out = features_joined(copies_to_all(out_share, "tp"))
    return (layer_out, new_state, new_conv_state)


def solution(mesh):
    split = Mesh(mesh.devices.reshape(16, 2, mesh.shape["tp"]), ("ep_0", "ep_1", "tp"))
    in_specs = (
        P(EP, None),
        P(EP, "tp"),
        P(EP, None, "tp"),
        P(),
        P(EP, "tp"),
        P(EP, "tp"),
        P(None, "tp"),
        P("tp", None, None),
        P("tp", None, None),
        P("tp"),
        P("tp", EP),
        P(),
        P(),
        P(EP, None),
        P(EP, None, "tp"),
        P(EP, None, "tp"),
        P(EP, "tp", None),
        P(EP, "tp"),
        P(EP, "tp"),
        P("tp", EP),
        P(),
    )
    out_specs = (P(EP, None), P(EP, "tp"), P(EP, None, "tp"))
    return jax.shard_map(
        on_device, mesh=split, in_specs=in_specs, out_specs=out_specs, check_vma=False
    )
```

```python
import jax
import jax.numpy as jnp
from jax import lax
from jax.experimental import pallas as pl
from jax.experimental.pallas import tpu as pltpu
from jax.sharding import Mesh
from jax.sharding import PartitionSpec as P

TOP_K = 2
EP = ("far", "near", "core")


epsilon = 1e-06
decay_scale = 8.0


def exchange(pieces, axis):
    return lax.all_to_all(pieces, axis, split_axis=0, concat_axis=0, tiled=True)


def copies_to_all(value, axis):
    return exchange(jnp.broadcast_to(value, (lax.axis_size(axis), *value.shape)), axis)


def features_joined(pieces):
    devices, count, share = pieces.shape
    return pieces.swapaxes(0, 1).reshape(count, devices * share)


def rms_scale(rows, gain):
    values = rows.astype(jnp.float32)
    inverse = lax.rsqrt(jnp.mean(values * values, axis=-1, keepdims=True) + epsilon)
    return (values * inverse * gain).astype(jnp.bfloat16)


def dot(left, right):
    return jnp.dot(left, right, preferred_element_type=jnp.float32)


def vmem():
    return pl.BlockSpec(memory_space=pltpu.VMEM)


def block_kernel(rows_ref, mine_ref, theirs_ref, out_ref):
    blocks = rows_ref.shape[0] // 2
    sources, items, _ = out_ref.shape
    half = items // 2
    for side in range(2):
        rows = jnp.concatenate([rows_ref[2 * b + side] for b in range(blocks)], axis=1)
        depth = rows.shape[1] // 2
        sums = dot(rows[:, :depth], mine_ref[...]) + dot(rows[:, depth:], theirs_ref[...])
        sums = sums.astype(jnp.bfloat16)
        for source in range(sources):
            out_ref[source, side * half : (side + 1) * half, :] = sums[source * half : (source + 1) * half]


def block_product(rows, mine, theirs, far, items):
    columns = mine.shape[1]
    return pl.pallas_call(
        block_kernel,
        out_shape=jax.ShapeDtypeStruct((far, items, columns), jnp.bfloat16),
        in_specs=[vmem()] * 3,
        out_specs=vmem(),
        compiler_params=pltpu.CompilerParams(vmem_limit_bytes=16 * 1024 * 1024),
        cost_estimate=pl.CostEstimate(flops=4 * rows.size * columns, bytes_accessed=2 * (rows.size + 2 * mine.size), transcendentals=0),
    )(rows, mine, theirs)


ROOMY = 61 * 1024 * 1024


def output_kernel(rows_ref, whole_hbm, out_ref, weight_ref, sems):
    channels = rows_ref.shape[1]
    chips = out_ref.shape[0]
    steps = 4
    owners = 2 * chips // steps
    copies = [
        pltpu.make_async_copy(
            whole_hbm.at[pl.ds(i * owners, owners), pl.ds(0, channels)],
            weight_ref.at[pl.ds(i * owners, owners)],
            sems.at[i],
        )
        for i in range(steps)
    ]
    for copy in copies:
        copy.start()
    rows = rows_ref[...]
    for z in range(chips):
        if z % (chips // steps) == 0:
            copies[z // (chips // steps)].wait()
        weight = jnp.concatenate([weight_ref[2 * z], weight_ref[2 * z + 1]], axis=1)
        out_ref[z] = dot(rows, weight).astype(jnp.bfloat16)


def output_product(rows, whole):
    owners, _, lanes = whole.shape
    channels = rows.shape[1]
    return pl.pallas_call(
        output_kernel,
        out_shape=jax.ShapeDtypeStruct((owners // 2, rows.shape[0], 2 * lanes), jnp.bfloat16),
        in_specs=[vmem(), pl.BlockSpec(memory_space=pl.ANY)],
        out_specs=vmem(),
        scratch_shapes=[pltpu.VMEM((owners, channels, lanes), whole.dtype), pltpu.SemaphoreType.DMA((4,))],
        compiler_params=pltpu.CompilerParams(vmem_limit_bytes=ROOMY),
        cost_estimate=pl.CostEstimate(flops=2 * rows.size * owners * lanes, bytes_accessed=2 * owners * channels * lanes, transcendentals=0),
    )(rows, whole)


def experts_kernel(pieces_ref, gain_ref, gate_hbm, up_hbm, down_hbm, whole_hbm, out_ref, own_ref, gate_ref, up_ref, down_ref, dense_ref, sems):
    chips, count, share = pieces_ref.shape
    depth = share // 2
    dense_at = whole_hbm.shape[1] - 3 * depth
    owners = whole_hbm.shape[0]
    copies = [
        pltpu.make_async_copy(source, target, sems.at[i])
        for i, (source, target) in enumerate(
            (
                (gate_hbm, gate_ref),
                (up_hbm, up_ref),
                (whole_hbm.at[pl.ds(0, owners), pl.ds(dense_at, 3 * depth)], dense_ref),
                (down_hbm, down_ref),
            )
        )
    ]
    for copy in copies:
        copy.start()
    slots = count - own_ref.shape[0]
    squares = jnp.zeros((count, share), jnp.float32)
    for z in range(chips):
        values = pieces_ref[z].astype(jnp.float32)
        squares = squares + values * values
    mean = jnp.sum(squares, axis=1, keepdims=True) / (chips * share)
    inverse = lax.rsqrt(mean + epsilon)
    for copy in copies[:2]:
        copy.wait()
    routed = jnp.zeros((slots, share), jnp.float32)
    for z in range(chips):
        at = pl.ds(z * share, share)
        rows = (pieces_ref[z].astype(jnp.float32) * inverse * gain_ref[:, at]).astype(jnp.bfloat16)
        routed = routed + dot(rows[:slots], jnp.concatenate([gate_ref[at, :], up_ref[at, :]], axis=1))
        own_ref[:, at] = rows[slots:]
    half = share // 2
    routed_act = (jax.nn.silu(routed[:, :half]) * routed[:, half:]).astype(jnp.bfloat16)
    copies[2].wait()
    dense = jnp.zeros((count - slots, share), jnp.float32)
    for z in range(chips):
        maps = [
            jnp.concatenate([dense_ref[2 * z + c, i * depth : (i + 1) * depth] for c in range(2)], axis=0)
            for i in range(2)
        ]
        dense = dense + dot(own_ref[:, pl.ds(z * share, share)], jnp.concatenate(maps, axis=1))
    dense_act = (jax.nn.silu(dense[:, :half]) * dense[:, half:]).astype(jnp.bfloat16)
    copies[3].wait()
    for z in range(chips):
        out_ref[z, :slots, :] = dot(routed_act, down_ref[:, pl.ds(z * share, share)]).astype(jnp.bfloat16)
        weight = jnp.concatenate([dense_ref[2 * z + c, 2 * depth :] for c in range(2)], axis=1)
        out_ref[z, slots:, :] = dot(dense_act, weight).astype(jnp.bfloat16)


def experts_product(pieces, gain, gate, up, down, whole, own_rows):
    chips, count, share = pieces.shape
    owners, _, lanes = whole.shape
    anywhere = pl.BlockSpec(memory_space=pl.ANY)
    weights = (gate, up, down)
    return pl.pallas_call(
        experts_kernel,
        out_shape=(
            jax.ShapeDtypeStruct(pieces.shape, jnp.bfloat16),
            jax.ShapeDtypeStruct((own_rows, chips * share), jnp.bfloat16),
        ),
        in_specs=[vmem(), vmem(), *([anywhere] * 4)],
        out_specs=(vmem(), vmem()),
        scratch_shapes=[
            *(pltpu.VMEM(w.shape, w.dtype) for w in weights),
            pltpu.VMEM((owners, 3 * lanes, lanes), whole.dtype),
            pltpu.SemaphoreType.DMA((4,)),
        ],
        compiler_params=pltpu.CompilerParams(vmem_limit_bytes=ROOMY),
        cost_estimate=pl.CostEstimate(flops=6 * count * gate.size, bytes_accessed=12 * gate.size, transcendentals=0),
    )(pieces, gain, *weights, whole)


def on_device(
    tokens,
    recur_state,
    conv_state,
    mix_gain,
    in_weight,
    gate_weight,
    conv_taps,
    recur_gate_blocks,
    input_gate_blocks,
    decay_rate,
    out_weight,
    ffn_gain,
    router_weight,
    routes,
    expert_gate,
    expert_up,
    expert_down,
    dense_gate,
    dense_up,
    dense_down,
    branch_gate,
):
    batch_rows, width = tokens.shape
    depth, channels = in_weight.shape
    columns = lax.axis_size("tp")
    share = width // columns
    far, near = lax.axis_size("far"), lax.axis_size("near")
    core = lax.axis_index("core")
    column = lax.axis_index("tp")
    swap = lambda value: lax.ppermute(value, "core", [(0, 1), (1, 0)])
    whole = lax.all_gather(jnp.concatenate([out_weight, dense_gate, dense_up, dense_down], axis=0), EP)
    normed = rms_scale(tokens, mix_gain)
    half = batch_rows // 2
    split_rows = normed.reshape(2, half, far, near, 2, depth)
    block, side = column // 2, column % 2
    block_near = (lax.axis_index("near") + block % near) % near
    block_core = jnp.where(block < near, core, 1 - core)
    sent = lax.dynamic_slice(
        split_rows, (side, 0, 0, block_near, block_core, 0), (1, half, far, 1, 1, depth)
    ).reshape(half, far, depth)
    came = exchange(sent.swapaxes(0, 1), "far").reshape(far * half, depth)
    block_rows = copies_to_all(came, "tp")
    both_weights = jnp.concatenate([in_weight, gate_weight], axis=1)
    from_near = lambda k: lax.ppermute(both_weights, "near", [(i, (i - k) % near) for i in range(near)])
    others = [from_near(k) for k in range(1, near)]
    block_mine = jnp.concatenate([both_weights, *others], axis=0)
    block_theirs = swap(block_mine)
    partial_sums = block_product(block_rows, block_mine, block_theirs, far, batch_rows)
    sent_back = exchange(partial_sums, "far")
    both_sums = sent_back.astype(jnp.float32).sum(axis=0)
    x_branch = both_sums[:, :channels].astype(jnp.bfloat16)
    gate_branch = both_sums[:, channels:].astype(jnp.bfloat16)
    window = jnp.concatenate([conv_state, x_branch[:, None, :]], axis=1)
    conv_out = jnp.sum(window.astype(jnp.float32) * conv_taps[None], axis=1).astype(jnp.bfloat16)
    new_conv_state = window[:, 1:, :]
    blocks = conv_out.reshape(batch_rows, recur_gate_blocks.shape[0], recur_gate_blocks.shape[1])

    def block_gate(maps):
        sums = jnp.einsum("bhi,hij->bhj", blocks, maps, preferred_element_type=jnp.float32)
        return jax.nn.sigmoid(sums.reshape(batch_rows, channels))

    recur_gate = block_gate(recur_gate_blocks)
    input_gate = block_gate(input_gate_blocks)
    log_decay = -decay_scale * recur_gate * decay_rate
    new_state = jnp.exp(log_decay) * recur_state + jnp.sqrt(
        -jnp.expm1(2.0 * log_decay)
    ) * input_gate * conv_out.astype(jnp.float32)
    mixer_rows = (new_state * jax.nn.gelu(gate_branch.astype(jnp.float32))).astype(jnp.bfloat16)
    own_tokens = lax.dynamic_slice_in_dim(tokens, column * share, share, 1)
    mixer_part = output_product(mixer_rows, whole)
    mixed_share = exchange(mixer_part, "tp").astype(jnp.float32).sum(axis=0)
    resid_share = (own_tokens.astype(jnp.float32) + mixed_share).astype(jnp.bfloat16)

    experts = router_weight.shape[1]
    capacity = 2 * batch_rows * TOP_K // experts
    flat_ids = routes.reshape(batch_rows * TOP_K)
    onehot = (
        flat_ids[:, None] == lax.broadcasted_iota(jnp.int32, (batch_rows * TOP_K, experts), 1)
    ).astype(jnp.int32)
    rank = jnp.sum((jnp.cumsum(onehot, axis=0) - onehot) * onehot, axis=1)
    slot_of = (flat_ids * capacity + rank).reshape(batch_rows, TOP_K)
    slot_rows = lax.broadcasted_iota(jnp.int32, (experts * capacity, batch_rows), 0)
    slot_cols = lax.broadcasted_iota(jnp.int32, (batch_rows, experts * capacity), 1)
    dispatch = jnp.zeros((experts * capacity, batch_rows), jnp.bfloat16)
    for pick in range(TOP_K):
        dispatch = dispatch + (slot_rows == slot_of[None, :, pick]).astype(jnp.bfloat16)

    outgoing = dot(dispatch, resid_share).astype(jnp.bfloat16).reshape(experts, capacity, share)
    arrived = exchange(outgoing, EP)
    sources, items, _ = arrived.shape
    slots = sources * items
    shares = jnp.concatenate([arrived.reshape(slots, share), resid_share], axis=0)
    parts_cut, normed_ffn = experts_product(
        copies_to_all(shares, "tp"),
        ffn_gain.reshape(1, width),
        expert_gate[0],
        expert_up[0],
        expert_down[0],
        whole,
        batch_rows,
    )
    sums = exchange(parts_cut, "tp").astype(jnp.float32).sum(axis=0)
    total, dense_share = sums[:slots].astype(jnp.bfloat16), sums[slots:]

    router_logits = dot(normed_ffn, router_weight)
    expert_ids = lax.broadcasted_iota(jnp.int32, (batch_rows, TOP_K, experts), 2)
    picked = jnp.sum(
        jnp.where(routes[:, :, None] == expert_ids, router_logits[:, None, :], 0.0), axis=2
    )
    route_weight = jax.nn.sigmoid(picked - picked[:, ::-1]).astype(jnp.bfloat16)
    combine = jnp.zeros((batch_rows, experts * capacity), jnp.bfloat16)
    for pick in range(TOP_K):
        combine = combine + jnp.where(
            slot_cols == slot_of[:, pick : pick + 1],
            route_weight[:, pick : pick + 1],
            jnp.zeros((), jnp.bfloat16),
        )
    branch_weight = jax.nn.sigmoid(dot(normed_ffn, branch_gate))

    returned = exchange(total.reshape(sources, items, share), EP)
    moe = dot(combine, returned.reshape(experts * capacity, share))
    out_share = (
        resid_share.astype(jnp.float32) + moe + branch_weight[:, None] * dense_share
    ).astype(jnp.bfloat16)
    layer_out = features_joined(copies_to_all(out_share, "tp"))
    return (layer_out, new_state, new_conv_state)


def solution(mesh):
    split = Mesh(mesh.devices.reshape(4, 4, 2, mesh.shape["tp"]), (*EP, "tp"))
    in_specs = (
        P(EP, None),
        P(EP, "tp"),
        P(EP, None, "tp"),
        P(),
        P(EP, "tp"),
        P(EP, "tp"),
        P(None, "tp"),
        P("tp", None, None),
        P("tp", None, None),
        P("tp"),
        P("tp", EP),
        P(),
        P(),
        P(EP, None),
        P(EP, None, "tp"),
        P(EP, None, "tp"),
        P(EP, "tp", None),
        P(EP, "tp"),
        P(EP, "tp"),
        P("tp", EP),
        P(),
    )
    out_specs = (P(EP, None), P(EP, "tp"), P(EP, None, "tp"))

    return jax.shard_map(on_device, mesh=split, in_specs=in_specs, out_specs=out_specs, check_vma=False)
```

```python
import jax
import jax.numpy as jnp
from jax import lax
from jax.experimental import pallas as pl
from jax.experimental.pallas import tpu as pltpu
from jax.sharding import Mesh
from jax.sharding import PartitionSpec as P

TOP_K = 2
EP = ("far", "near", "core")


epsilon = 1e-06
decay_scale = 8.0


def exchange(pieces, axis):
    return lax.all_to_all(pieces, axis, split_axis=0, concat_axis=0, tiled=True)


def copies_to_all(value, axis):
    return exchange(jnp.broadcast_to(value, (lax.axis_size(axis), *value.shape)), axis)


def features_joined(pieces):
    devices, count, share = pieces.shape
    return pieces.swapaxes(0, 1).reshape(count, devices * share)


def rms_scale(rows, gain):
    values = rows.astype(jnp.float32)
    inverse = lax.rsqrt(jnp.mean(values * values, axis=-1, keepdims=True) + epsilon)
    return (values * inverse * gain).astype(jnp.bfloat16)


def dot(left, right):
    return jnp.dot(left, right, preferred_element_type=jnp.float32)


def vmem():
    return pl.BlockSpec(memory_space=pltpu.VMEM)


def block_kernel(rows_ref, mine_ref, theirs_ref, out_ref):
    blocks = rows_ref.shape[0] // 2
    sources, items, _ = out_ref.shape
    half = items // 2
    for side in range(2):
        rows = jnp.concatenate([rows_ref[2 * b + side] for b in range(blocks)], axis=1)
        depth = rows.shape[1] // 2
        sums = dot(rows[:, :depth], mine_ref[...]) + dot(rows[:, depth:], theirs_ref[...])
        sums = sums.astype(jnp.bfloat16)
        for source in range(sources):
            out_ref[source, side * half : (side + 1) * half, :] = sums[source * half : (source + 1) * half]


def block_product(rows, mine, theirs, far, items):
    columns = mine.shape[1]
    return pl.pallas_call(
        block_kernel,
        out_shape=jax.ShapeDtypeStruct((far, items, columns), jnp.bfloat16),
        in_specs=[vmem()] * 3,
        out_specs=vmem(),
        compiler_params=pltpu.CompilerParams(vmem_limit_bytes=16 * 1024 * 1024),
        cost_estimate=pl.CostEstimate(flops=4 * rows.size * columns, bytes_accessed=2 * (rows.size + 2 * mine.size), transcendentals=0),
    )(rows, mine, theirs)


ROOMY = 60 * 1024 * 1024


def output_kernel(rows_ref, whole_hbm, out_ref, weight_ref, sems):
    channels = rows_ref.shape[1]
    chips = out_ref.shape[0]
    steps = 4
    owners = 2 * chips // steps
    copies = [
        pltpu.make_async_copy(
            whole_hbm.at[pl.ds(i * owners, owners), pl.ds(0, channels)],
            weight_ref.at[pl.ds(i * owners, owners)],
            sems.at[i],
        )
        for i in range(steps)
    ]
    for copy in copies:
        copy.start()
    rows = rows_ref[...]
    for z in range(chips):
        if z % (chips // steps) == 0:
            copies[z // (chips // steps)].wait()
        weight = jnp.concatenate([weight_ref[2 * z], weight_ref[2 * z + 1]], axis=1)
        out_ref[z] = dot(rows, weight).astype(jnp.bfloat16)


def output_product(rows, whole):
    owners, _, lanes = whole.shape
    channels = rows.shape[1]
    return pl.pallas_call(
        output_kernel,
        out_shape=jax.ShapeDtypeStruct((owners // 2, rows.shape[0], 2 * lanes), jnp.bfloat16),
        in_specs=[vmem(), pl.BlockSpec(memory_space=pl.ANY)],
        out_specs=vmem(),
        scratch_shapes=[pltpu.VMEM((owners, channels, lanes), whole.dtype), pltpu.SemaphoreType.DMA((4,))],
        compiler_params=pltpu.CompilerParams(vmem_limit_bytes=ROOMY),
        cost_estimate=pl.CostEstimate(flops=2 * rows.size * owners * lanes, bytes_accessed=2 * owners * channels * lanes, transcendentals=0),
    )(rows, whole)


def fetch_kernel(gate_hbm, up_hbm, down_hbm, whole_hbm, both_ref, down_ref, dense_ref, sems):
    half = gate_hbm.shape[1]
    owners, rows, _ = dense_ref.shape
    copies = [
        pltpu.make_async_copy(source, target, sems.at[i])
        for i, (source, target) in enumerate(
            (
                (gate_hbm, both_ref.at[:, pl.ds(0, half)]),
                (up_hbm, both_ref.at[:, pl.ds(half, half)]),
                (whole_hbm.at[pl.ds(0, owners), pl.ds(whole_hbm.shape[1] - rows, rows)], dense_ref),
                (down_hbm, down_ref),
            )
        )
    ]
    for copy in copies:
        copy.start()
    for copy in copies:
        copy.wait()


def fetch_weights(gate, up, down, whole, dense_rows):
    owners, _, lanes = whole.shape
    return pl.pallas_call(
        fetch_kernel,
        out_shape=(
            jax.ShapeDtypeStruct((gate.shape[0], 2 * gate.shape[1]), gate.dtype),
            jax.ShapeDtypeStruct(down.shape, down.dtype),
            jax.ShapeDtypeStruct((owners, dense_rows, lanes), whole.dtype),
        ),
        in_specs=[pl.BlockSpec(memory_space=pl.ANY)] * 4,
        out_specs=(vmem(),) * 3,
        scratch_shapes=[pltpu.SemaphoreType.DMA((4,))],
        compiler_params=pltpu.CompilerParams(vmem_limit_bytes=54 * 1024 * 1024),
        cost_estimate=pl.CostEstimate(flops=40_000_000, bytes_accessed=6 * gate.size, transcendentals=0),
    )(gate, up, down, whole)


def experts_kernel(pieces_ref, gain_ref, both_ref, down_ref, dense_ref, maps_ref, picks_ref, places_ref, out_ref, combine_ref, branch_ref):
    chips, count, share = pieces_ref.shape
    depth = share // 2
    slots = down_ref.shape[0]
    rows_own = count - slots
    squares = jnp.zeros((count, share), jnp.float32)
    for z in range(chips):
        values = pieces_ref[z].astype(jnp.float32)
        squares = squares + values * values
    mean = jnp.sum(squares, axis=1, keepdims=True) / (chips * share)
    inverse = lax.rsqrt(mean + epsilon)
    routed = jnp.zeros((slots, share), jnp.float32)
    dense = jnp.zeros((rows_own, share), jnp.float32)
    logits = jnp.zeros((rows_own, maps_ref.shape[0]), jnp.float32)
    for z in range(chips):
        at = pl.ds(z * share, share)
        rows = (pieces_ref[z].astype(jnp.float32) * inverse * gain_ref[:, at]).astype(jnp.bfloat16)
        routed = routed + dot(rows[:slots], both_ref[at, :])
        weights = [
            jnp.concatenate([dense_ref[2 * z + c, i * depth : (i + 1) * depth] for c in range(2)], axis=0)
            for i in range(2)
        ]
        dense = dense + dot(rows[slots:], jnp.concatenate(weights, axis=1))
        logits = logits + lax.dot_general(
            rows[slots:], maps_ref[:, at], (((1,), (1,)), ((), ())), preferred_element_type=jnp.float32
        )
    half = share // 2
    routed_act = (jax.nn.silu(routed[:, :half]) * routed[:, half:]).astype(jnp.bfloat16)
    dense_act = (jax.nn.silu(dense[:, :half]) * dense[:, half:]).astype(jnp.bfloat16)
    for z in range(chips):
        out_ref[z, :slots, :] = dot(routed_act, down_ref[:, pl.ds(z * share, share)]).astype(jnp.bfloat16)
        weight = jnp.concatenate([dense_ref[2 * z + c, 2 * depth :] for c in range(2)], axis=1)
        out_ref[z, slots:, :] = dot(dense_act, weight).astype(jnp.bfloat16)

    experts = maps_ref.shape[0] - 8
    column = lax.broadcasted_iota(jnp.int32, logits.shape, 1)

    def of_column(index):
        return jnp.sum(jnp.where(column == index, logits, 0.0), axis=1, keepdims=True)

    picked = [of_column(picks_ref[:, k : k + 1]) for k in range(TOP_K)]
    place = lax.broadcasted_iota(jnp.int32, (rows_own, combine_ref.shape[1]), 1)
    total = jnp.zeros((rows_own, combine_ref.shape[1]), jnp.float32)
    for k in range(TOP_K):
        weight = jax.nn.sigmoid(picked[k] - picked[1 - k]).astype(jnp.bfloat16).astype(jnp.float32)
        total = total + jnp.where(place == places_ref[:, k : k + 1], weight, 0.0)
    combine_ref[...] = total.astype(jnp.bfloat16)
    branch_ref[...] = jnp.broadcast_to(jax.nn.sigmoid(of_column(experts)), branch_ref.shape)


def experts_product(pieces, gain, both, down, dense, maps, picks, places):
    _, count, share = pieces.shape
    own_rows = picks.shape[0]
    return pl.pallas_call(
        experts_kernel,
        out_shape=(
            jax.ShapeDtypeStruct(pieces.shape, jnp.bfloat16),
            jax.ShapeDtypeStruct((own_rows, count - own_rows), jnp.bfloat16),
            jax.ShapeDtypeStruct((own_rows, share), jnp.float32),
        ),
        in_specs=[vmem()] * 8,
        out_specs=(vmem(),) * 3,
        compiler_params=pltpu.CompilerParams(vmem_limit_bytes=16 * 1024 * 1024),
        cost_estimate=pl.CostEstimate(flops=3 * count * both.size, bytes_accessed=6 * both.size, transcendentals=0),
    )(pieces, gain, both, down, dense, maps, picks, places)


def on_device(
    tokens,
    recur_state,
    conv_state,
    mix_gain,
    in_weight,
    gate_weight,
    conv_taps,
    recur_gate_blocks,
    input_gate_blocks,
    decay_rate,
    out_weight,
    ffn_gain,
    router_weight,
    routes,
    expert_gate,
    expert_up,
    expert_down,
    dense_gate,
    dense_up,
    dense_down,
    branch_gate,
):
    batch_rows, width = tokens.shape
    depth, channels = in_weight.shape
    columns = lax.axis_size("tp")
    share = width // columns
    far, near = lax.axis_size("far"), lax.axis_size("near")
    core = lax.axis_index("core")
    column = lax.axis_index("tp")
    swap = lambda value: lax.ppermute(value, "core", [(0, 1), (1, 0)])
    whole = lax.all_gather(jnp.concatenate([out_weight, dense_gate, dense_up, dense_down], axis=0), EP)
    normed = rms_scale(tokens, mix_gain)
    half = batch_rows // 2
    split_rows = normed.reshape(2, half, far, near, 2, depth)
    block, side = column // 2, column % 2
    block_near = (lax.axis_index("near") + block % near) % near
    block_core = jnp.where(block < near, core, 1 - core)
    sent = lax.dynamic_slice(
        split_rows, (side, 0, 0, block_near, block_core, 0), (1, half, far, 1, 1, depth)
    ).reshape(half, far, depth)
    came = exchange(sent.swapaxes(0, 1), "far").reshape(far * half, depth)
    experts = router_weight.shape[1]
    capacity = 2 * batch_rows * TOP_K // experts
    flat_ids = routes.reshape(batch_rows * TOP_K)
    onehot = (
        flat_ids[:, None] == lax.broadcasted_iota(jnp.int32, (batch_rows * TOP_K, experts), 1)
    ).astype(jnp.int32)
    rank = jnp.sum((jnp.cumsum(onehot, axis=0) - onehot) * onehot, axis=1)
    slot_of = (flat_ids * capacity + rank).reshape(batch_rows, TOP_K)
    slots = experts * capacity
    slot_rows = lax.broadcasted_iota(jnp.int32, (slots, batch_rows), 0)
    dispatch = sum((slot_rows == slot_of[None, :, pick]).astype(jnp.bfloat16) for pick in range(TOP_K))
    maps = jnp.concatenate(
        [router_weight.T, branch_gate.reshape(1, width), jnp.zeros((7, width), jnp.bfloat16)], axis=0
    )
    own_tokens = lax.dynamic_slice_in_dim(tokens, column * share, share, 1)
    came, dispatch, slot_of, maps, own_tokens = lax.optimization_barrier(
        (came, dispatch, slot_of, maps, own_tokens)
    )

    block_rows = copies_to_all(came, "tp")
    both_weights = jnp.concatenate([in_weight, gate_weight], axis=1)
    from_near = lambda k: lax.ppermute(both_weights, "near", [(i, (i - k) % near) for i in range(near)])
    others = [from_near(k) for k in range(1, near)]
    block_mine = jnp.concatenate([both_weights, *others], axis=0)
    block_theirs = swap(block_mine)
    partial_sums = block_product(block_rows, block_mine, block_theirs, far, batch_rows)
    sent_back = exchange(partial_sums, "far")
    both_sums = sent_back.astype(jnp.float32).sum(axis=0)
    x_branch = both_sums[:, :channels].astype(jnp.bfloat16)
    gate_branch = both_sums[:, channels:].astype(jnp.bfloat16)
    window = jnp.concatenate([conv_state, x_branch[:, None, :]], axis=1)
    conv_out = jnp.sum(window.astype(jnp.float32) * conv_taps[None], axis=1).astype(jnp.bfloat16)
    new_conv_state = window[:, 1:, :]
    blocks = conv_out.reshape(batch_rows, recur_gate_blocks.shape[0], recur_gate_blocks.shape[1])

    def block_gate(maps):
        sums = jnp.einsum("bhi,hij->bhj", blocks, maps, preferred_element_type=jnp.float32)
        return jax.nn.sigmoid(sums.reshape(batch_rows, channels))

    recur_gate = block_gate(recur_gate_blocks)
    input_gate = block_gate(input_gate_blocks)
    log_decay = -decay_scale * recur_gate * decay_rate
    new_state = jnp.exp(log_decay) * recur_state + jnp.sqrt(
        -jnp.expm1(2.0 * log_decay)
    ) * input_gate * conv_out.astype(jnp.float32)
    mixer_rows = (new_state * jax.nn.gelu(gate_branch.astype(jnp.float32))).astype(jnp.bfloat16)
    mixer_rows, new_conv_state = lax.optimization_barrier((mixer_rows, new_conv_state))
    mixer_part = output_product(mixer_rows, whole)
    mixed_share = exchange(mixer_part, "tp").astype(jnp.float32).sum(axis=0)
    resid_share = (own_tokens.astype(jnp.float32) + mixed_share).astype(jnp.bfloat16)

    outgoing = dot(dispatch, resid_share).astype(jnp.bfloat16)
    arrived = exchange(outgoing.reshape(experts, capacity, share), EP).reshape(slots, share)
    fetched = fetch_weights(expert_gate[0], expert_up[0], expert_down[0], whole, 3 * depth)
    arrived, fetched = lax.optimization_barrier((arrived, fetched))
    shares = jnp.concatenate([arrived, resid_share], axis=0)
    parts_cut, combine, branch_weight = experts_product(
        copies_to_all(shares, "tp"), ffn_gain.reshape(1, width), *fetched, maps, routes, slot_of
    )
    sums = exchange(parts_cut, "tp").astype(jnp.float32).sum(axis=0)
    total, dense_share = sums[:slots].astype(jnp.bfloat16), sums[slots:]

    returned = exchange(total.reshape(experts, capacity, share), EP)
    moe = dot(combine, returned.reshape(slots, share))
    out_share = (
        resid_share.astype(jnp.float32) + moe + branch_weight * dense_share
    ).astype(jnp.bfloat16)
    layer_out = features_joined(copies_to_all(out_share, "tp"))
    return (layer_out, new_state, new_conv_state)


def solution(mesh):
    split = Mesh(mesh.devices.reshape(4, 4, 2, mesh.shape["tp"]), (*EP, "tp"))
    in_specs = (
        P(EP, None),
        P(EP, "tp"),
        P(EP, None, "tp"),
        P(),
        P(EP, "tp"),
        P(EP, "tp"),
        P(None, "tp"),
        P("tp", None, None),
        P("tp", None, None),
        P("tp"),
        P("tp", EP),
        P(),
        P(),
        P(EP, None),
        P(EP, None, "tp"),
        P(EP, None, "tp"),
        P(EP, "tp", None),
        P(EP, "tp"),
        P(EP, "tp"),
        P("tp", EP),
        P(),
    )
    out_specs = (P(EP, None), P(EP, "tp"), P(EP, None, "tp"))

    return jax.shard_map(on_device, mesh=split, in_specs=in_specs, out_specs=out_specs, check_vma=False)
```

```python
import jax
import jax.numpy as jnp
from jax import lax
from jax.experimental import pallas as pl
from jax.experimental.pallas import tpu as pltpu
from jax.sharding import Mesh
from jax.sharding import PartitionSpec as P

TOP_K = 2
EP = ("far", "near", "core")


epsilon = 1e-06
decay_scale = 8.0


def exchange(pieces, axis):
    return lax.all_to_all(pieces, axis, split_axis=0, concat_axis=0, tiled=True)


def copies_to_all(value, axis):
    return exchange(jnp.broadcast_to(value, (lax.axis_size(axis), *value.shape)), axis)


def features_joined(pieces):
    devices, count, share = pieces.shape
    return pieces.swapaxes(0, 1).reshape(count, devices * share)


def rms_scale(rows, gain):
    values = rows.astype(jnp.float32)
    inverse = lax.rsqrt(jnp.mean(values * values, axis=-1, keepdims=True) + epsilon)
    return (values * inverse * gain).astype(jnp.bfloat16)


def dot(left, right):
    return jnp.dot(left, right, preferred_element_type=jnp.float32)


def vmem():
    return pl.BlockSpec(memory_space=pltpu.VMEM)


def block_kernel(rows_ref, mine_ref, theirs_ref, out_ref):
    blocks = rows_ref.shape[0] // 2
    sources, items, _ = out_ref.shape
    half = items // 2
    for side in range(2):
        rows = jnp.concatenate([rows_ref[2 * b + side] for b in range(blocks)], axis=1)
        depth = rows.shape[1] // 2
        sums = dot(rows[:, :depth], mine_ref[...]) + dot(rows[:, depth:], theirs_ref[...])
        sums = sums.astype(jnp.bfloat16)
        for source in range(sources):
            out_ref[source, side * half : (side + 1) * half, :] = sums[source * half : (source + 1) * half]


def block_product(rows, mine, theirs, far, items):
    columns = mine.shape[1]
    return pl.pallas_call(
        block_kernel,
        out_shape=jax.ShapeDtypeStruct((far, items, columns), jnp.bfloat16),
        in_specs=[vmem()] * 3,
        out_specs=vmem(),
        compiler_params=pltpu.CompilerParams(vmem_limit_bytes=16 * 1024 * 1024),
        cost_estimate=pl.CostEstimate(flops=4 * rows.size * columns, bytes_accessed=2 * (rows.size + 2 * mine.size), transcendentals=0),
    )(rows, mine, theirs)


ROOMY = 60 * 1024 * 1024


def output_kernel(rows_hbm, whole_hbm, out_hbm, rows_ref, weight_ref, out_ref, row_sem, in_sems, out_sems):
    channels = rows_ref.shape[1]
    chips = out_ref.shape[0]
    steps = in_sems.shape[0]
    each = chips // steps
    owners = 2 * each
    row_copy = pltpu.make_async_copy(rows_hbm, rows_ref, row_sem)
    row_copy.start()
    copies = [
        pltpu.make_async_copy(
            whole_hbm.at[pl.ds(i * owners, owners), pl.ds(0, channels)],
            weight_ref.at[pl.ds(i * owners, owners)],
            in_sems.at[i],
        )
        for i in range(steps)
    ]
    for copy in copies:
        copy.start()
    row_copy.wait()
    rows = rows_ref[...]
    results = []
    for i in range(steps):
        copies[i].wait()
        for z in range(i * each, (i + 1) * each):
            weight = jnp.concatenate([weight_ref[2 * z], weight_ref[2 * z + 1]], axis=1)
            out_ref[z] = dot(rows, weight).astype(jnp.bfloat16)
        result = pltpu.make_async_copy(
            out_ref.at[pl.ds(i * each, each)], out_hbm.at[pl.ds(i * each, each)], out_sems.at[i]
        )
        result.start()
        results.append(result)
    for result in results:
        result.wait()


def output_product(rows, whole):
    owners, _, lanes = whole.shape
    channels = rows.shape[1]
    out = jax.ShapeDtypeStruct((owners // 2, rows.shape[0], 2 * lanes), jnp.bfloat16)
    anywhere = pl.BlockSpec(memory_space=pl.ANY)
    steps = 4
    return pl.pallas_call(
        output_kernel,
        out_shape=out,
        in_specs=[anywhere, anywhere],
        out_specs=anywhere,
        scratch_shapes=[
            pltpu.VMEM(rows.shape, rows.dtype),
            pltpu.VMEM((owners, channels, lanes), whole.dtype),
            pltpu.VMEM(out.shape, out.dtype),
            pltpu.SemaphoreType.DMA,
            pltpu.SemaphoreType.DMA((steps,)),
            pltpu.SemaphoreType.DMA((steps,)),
        ],
        compiler_params=pltpu.CompilerParams(vmem_limit_bytes=ROOMY),
        cost_estimate=pl.CostEstimate(flops=2 * rows.size * owners * lanes, bytes_accessed=2 * owners * channels * lanes, transcendentals=0),
    )(rows, whole)


def experts_kernel(pieces_ref, gain_ref, maps_ref, facts_ref, gate_hbm, up_hbm, down_hbm, whole_hbm, out_ref, both_ref, down_ref, dense_ref, rows_ref, sems):
    chips, slots, share = pieces_ref.shape
    depth = share // 2
    owners, dense_rows, _ = dense_ref.shape
    copies = [
        pltpu.make_async_copy(source, target, sems.at[i])
        for i, (source, target) in enumerate(
            (
                (gate_hbm, both_ref.at[:, pl.ds(0, depth)]),
                (up_hbm, both_ref.at[:, pl.ds(depth, depth)]),
                (whole_hbm.at[pl.ds(0, owners), pl.ds(whole_hbm.shape[1] - dense_rows, dense_rows)], dense_ref),
                (down_hbm, down_ref),
            )
        )
    ]
    for copy in copies:
        copy.start()
    squares = jnp.zeros((slots, share), jnp.float32)
    for z in range(chips):
        values = pieces_ref[z].astype(jnp.float32)
        squares = squares + values * values
    mean = jnp.sum(squares, axis=1, keepdims=True) / (chips * share)
    inverse = lax.rsqrt(mean + epsilon)
    copies[0].wait()
    copies[1].wait()
    routed = jnp.zeros((slots, share), jnp.float32)
    dense = jnp.zeros((slots, share), jnp.float32)
    logits = jnp.zeros((slots, maps_ref.shape[0]), jnp.float32)
    for z in range(chips):
        at = pl.ds(z * share, share)
        rows = (pieces_ref[z].astype(jnp.float32) * inverse * gain_ref[:, at]).astype(jnp.bfloat16)
        rows_ref[z] = rows
        routed = routed + dot(rows, both_ref[at, :])
        logits = logits + lax.dot_general(
            rows, maps_ref[:, at], (((1,), (1,)), ((), ())), preferred_element_type=jnp.float32
        )
    copies[2].wait()
    for z in range(chips):
        weights = [
            jnp.concatenate([dense_ref[2 * z + c, i * depth : (i + 1) * depth] for c in range(2)], axis=0)
            for i in range(2)
        ]
        dense = dense + dot(rows_ref[z], jnp.concatenate(weights, axis=1))
    copies[3].wait()
    half = share // 2
    routed_act = (jax.nn.silu(routed[:, :half]) * routed[:, half:]).astype(jnp.bfloat16)
    dense_act = (jax.nn.silu(dense[:, :half]) * dense[:, half:]).astype(jnp.bfloat16)

    facts = facts_ref[...].astype(jnp.float32)
    column = lax.broadcasted_iota(jnp.int32, logits.shape, 1).astype(jnp.float32)

    def of_column(index):
        return jnp.sum(jnp.where(column == index, logits, 0.0), axis=1, keepdims=True)

    expert_weight = jax.nn.sigmoid(of_column(facts[:, 0:1]) - of_column(facts[:, 1:2]))
    expert_weight = expert_weight.astype(jnp.bfloat16).astype(jnp.float32)
    branch_weight = jax.nn.sigmoid(of_column(float(maps_ref.shape[0] - 8))) * facts[:, 2:3]
    for z in range(chips):
        weight = jnp.concatenate([dense_ref[2 * z + c, 2 * depth :] for c in range(2)], axis=1)
        part = expert_weight * dot(routed_act, down_ref[:, pl.ds(z * share, share)])
        out_ref[z] = (part + branch_weight * dot(dense_act, weight)).astype(jnp.bfloat16)


def experts_product(pieces, gain, maps, facts, gate, up, down, whole, dense_rows):
    owners, _, lanes = whole.shape
    anywhere = pl.BlockSpec(memory_space=pl.ANY)
    return pl.pallas_call(
        experts_kernel,
        out_shape=jax.ShapeDtypeStruct(pieces.shape, jnp.bfloat16),
        in_specs=[*([vmem()] * 4), *([anywhere] * 4)],
        out_specs=vmem(),
        scratch_shapes=[
            pltpu.VMEM((gate.shape[0], 2 * gate.shape[1]), gate.dtype),
            pltpu.VMEM(down.shape, down.dtype),
            pltpu.VMEM((owners, dense_rows, lanes), whole.dtype),
            pltpu.VMEM(pieces.shape, pieces.dtype),
            pltpu.SemaphoreType.DMA((4,)),
        ],
        compiler_params=pltpu.CompilerParams(vmem_limit_bytes=ROOMY),
        cost_estimate=pl.CostEstimate(flops=12 * pieces.shape[1] * gate.size, bytes_accessed=12 * gate.size, transcendentals=0),
    )(pieces, gain, maps, facts, gate, up, down, whole)


def on_device(
    tokens,
    recur_state,
    conv_state,
    mix_gain,
    in_weight,
    gate_weight,
    conv_taps,
    recur_gate_blocks,
    input_gate_blocks,
    decay_rate,
    out_weight,
    ffn_gain,
    router_weight,
    routes,
    expert_gate,
    expert_up,
    expert_down,
    dense_gate,
    dense_up,
    dense_down,
    branch_gate,
):
    batch_rows, width = tokens.shape
    depth, channels = in_weight.shape
    lanes = out_weight.shape[1]
    columns = lax.axis_size("tp")
    share = width // columns
    far, near = lax.axis_size("far"), lax.axis_size("near")
    core = lax.axis_index("core")
    column = lax.axis_index("tp")
    swap = lambda value: lax.ppermute(value, "core", [(0, 1), (1, 0)])
    whole = lax.all_gather(jnp.concatenate([out_weight, dense_gate, dense_up, dense_down], axis=0), EP)
    normed = rms_scale(tokens, mix_gain)
    half = batch_rows // 2
    split_rows = normed.reshape(2, half, far, near, 2, depth)
    block, side = column // 2, column % 2
    block_near = (lax.axis_index("near") + block % near) % near
    block_core = jnp.where(block < near, core, 1 - core)
    sent = lax.dynamic_slice(
        split_rows, (side, 0, 0, block_near, block_core, 0), (1, half, far, 1, 1, depth)
    ).reshape(half, far, depth)
    came = exchange(sent.swapaxes(0, 1), "far").reshape(far * half, depth)
    experts = router_weight.shape[1]
    capacity = 2 * batch_rows * TOP_K // experts
    flat_ids = routes.reshape(batch_rows * TOP_K)
    onehot = (
        flat_ids[:, None] == lax.broadcasted_iota(jnp.int32, (batch_rows * TOP_K, experts), 1)
    ).astype(jnp.int32)
    rank = jnp.sum((jnp.cumsum(onehot, axis=0) - onehot) * onehot, axis=1)
    slot_of = (flat_ids * capacity + rank).reshape(batch_rows, TOP_K)
    slots = experts * capacity
    slot_rows = lax.broadcasted_iota(jnp.int32, (slots, batch_rows), 0)
    picks = [(slot_rows == slot_of[None, :, pick]).astype(jnp.bfloat16) for pick in range(TOP_K)]
    dispatch = picks[0] + picks[1]
    lane = lax.broadcasted_iota(jnp.int32, (batch_rows, lanes), 1)
    facts = sum(
        dot(
            picks[k],
            jnp.where(
                lane == 0,
                routes[:, k : k + 1],
                jnp.where(lane == 1, routes[:, 1 - k : 2 - k], jnp.where(lane == 2, 1 - k, 0)),
            ).astype(jnp.bfloat16),
        )
        for k in range(TOP_K)
    ).astype(jnp.bfloat16)
    maps = jnp.concatenate(
        [router_weight.T, branch_gate.reshape(1, width), jnp.zeros((7, width), jnp.bfloat16)], axis=0
    )
    own_tokens = lax.dynamic_slice_in_dim(tokens, column * share, share, 1)
    came, dispatch, facts, maps, own_tokens = lax.optimization_barrier(
        (came, dispatch, facts, maps, own_tokens)
    )

    block_rows = copies_to_all(came, "tp")
    both_weights = jnp.concatenate([in_weight, gate_weight], axis=1)
    from_near = lambda k: lax.ppermute(both_weights, "near", [(i, (i - k) % near) for i in range(near)])
    others = [from_near(k) for k in range(1, near)]
    block_mine = jnp.concatenate([both_weights, *others], axis=0)
    block_theirs = swap(block_mine)
    partial_sums = block_product(block_rows, block_mine, block_theirs, far, batch_rows)
    sent_back = exchange(partial_sums, "far")
    both_sums = sent_back.astype(jnp.float32).sum(axis=0)
    x_branch = both_sums[:, :channels].astype(jnp.bfloat16)
    gate_branch = both_sums[:, channels:].astype(jnp.bfloat16)
    window = jnp.concatenate([conv_state, x_branch[:, None, :]], axis=1)
    conv_out = jnp.sum(window.astype(jnp.float32) * conv_taps[None], axis=1).astype(jnp.bfloat16)
    new_conv_state = window[:, 1:, :]
    blocks = conv_out.reshape(batch_rows, recur_gate_blocks.shape[0], recur_gate_blocks.shape[1])

    def block_gate(maps):
        sums = jnp.einsum("bhi,hij->bhj", blocks, maps, preferred_element_type=jnp.float32)
        return jax.nn.sigmoid(sums.reshape(batch_rows, channels))

    recur_gate = block_gate(recur_gate_blocks)
    input_gate = block_gate(input_gate_blocks)
    log_decay = -decay_scale * recur_gate * decay_rate
    new_state = jnp.exp(log_decay) * recur_state + jnp.sqrt(
        -jnp.expm1(2.0 * log_decay)
    ) * input_gate * conv_out.astype(jnp.float32)
    mixer_rows = (new_state * jax.nn.gelu(gate_branch.astype(jnp.float32))).astype(jnp.bfloat16)
    mixer_rows, new_conv_state = lax.optimization_barrier((mixer_rows, new_conv_state))
    mixer_part = output_product(mixer_rows, whole)
    mixed_share = exchange(mixer_part, "tp").astype(jnp.float32).sum(axis=0)
    resid_share = (own_tokens.astype(jnp.float32) + mixed_share).astype(jnp.bfloat16)

    outgoing = jnp.concatenate([dot(dispatch, resid_share).astype(jnp.bfloat16), facts], axis=1)
    arrived = exchange(outgoing.reshape(experts, capacity, -1), EP).reshape(slots, -1)
    arrived_share, arrived_facts = lax.optimization_barrier((arrived[:, :share], arrived[:, share:]))
    pieces = copies_to_all(arrived_share, "tp")
    parts_cut = experts_product(
        pieces,
        ffn_gain.reshape(1, width),
        maps,
        arrived_facts,
        expert_gate[0],
        expert_up[0],
        expert_down[0],
        whole,
        3 * depth,
    )
    total = exchange(parts_cut, "tp").astype(jnp.float32).sum(axis=0).astype(jnp.bfloat16)
    returned = exchange(total.reshape(experts, capacity, share), EP)
    branches = dot(dispatch.T, returned.reshape(slots, share))
    out_share = (resid_share.astype(jnp.float32) + branches).astype(jnp.bfloat16)
    layer_out = features_joined(copies_to_all(out_share, "tp"))
    return (layer_out, new_state, new_conv_state)


def solution(mesh):
    split = Mesh(mesh.devices.reshape(4, 4, 2, mesh.shape["tp"]), (*EP, "tp"))
    in_specs = (
        P(EP, None),
        P(EP, "tp"),
        P(EP, None, "tp"),
        P(),
        P(EP, "tp"),
        P(EP, "tp"),
        P(None, "tp"),
        P("tp", None, None),
        P("tp", None, None),
        P("tp"),
        P("tp", EP),
        P(),
        P(),
        P(EP, None),
        P(EP, None, "tp"),
        P(EP, None, "tp"),
        P(EP, "tp", None),
        P(EP, "tp"),
        P(EP, "tp"),
        P("tp", EP),
        P(),
    )
    out_specs = (P(EP, None), P(EP, "tp"), P(EP, None, "tp"))

    return jax.shard_map(on_device, mesh=split, in_specs=in_specs, out_specs=out_specs, check_vma=False)
```
